32 devices in a mesh: sp: 8 (over z, x), tp: 4 (over y, core).
Axes of the slice: x: 2, y: 2, z: 4, core: 2. Of those that a mesh axis runs over, the one named last changes fastest.
Arguments:
- resid: bfloat16 [6144, 2048], P(('sp', 'tp')), may hold values from -6 to 6
- queries: bfloat16 [6144, 1024], P('sp', 'tp'), may hold values from -160 to 160
- keys: bfloat16 [6144, 1024], P('sp', 'tp'), may hold values from -6 to 6
- values: bfloat16 [6144, 1024], P('sp', 'tp'), may hold values from -6 to 6
- cum_gate: float32 [6144, 16], P('sp', 'tp'), may hold values from -694 to 0, as said below
- out_weight: bfloat16 [1024, 2048], P('tp'), may hold values from -0.375 to 0.375
- norm_gain: float32 [2048], replicated, may hold values from 0.1 to 1.9
- gate_weight: bfloat16 [2048, 5504], P('sp', 'tp'), may hold values from -0.125 to 0.125
- up_weight: bfloat16 [2048, 5504], P('sp', 'tp'), may hold values from -0.125 to 0.125
- down_weight: bfloat16 [5504, 2048], P('tp', 'sp'), may hold values from -0.078125 to 0.078125
Outputs:
- layer_out: bfloat16 [6144, 2048], P(('sp', 'tp'))
The draws below stay inside these ranges and needn't reach their ends.
Inputs may be any that keep to these rules, and one draw needn't show every extreme that they name: `cum_gate`: each column is non-increasing along positions and starts at or below zero.
All inputs are finite; a program needn't handle non-finite values.
Results may differ from the reference program's by a relative error of at most 0.01.
Values may be sent and summed in bfloat16 or wider, within the bound.
A program may use at most 256 MiB of HBM per device.

```python
import jax
import jax.numpy as jnp
from jax import lax

D = 2048
HEAD_COUNT = 16
HEAD_DIM = 64
FF = 5504
TOK_DEV = 768
TOKEN_COUNT = 6144
N_SP = 8
N_TP = 4


def paired_rows(key):
    key_query, key_key = jax.random.split(jax.random.fold_in(key, 11))
    width = HEAD_COUNT * HEAD_DIM
    queries = 2.5 * jnp.clip(jax.random.normal(key_query, (TOKEN_COUNT, width), jnp.float32), -5.0, 5.0)
    keys = jnp.clip(jax.random.normal(key_key, (TOKEN_COUNT, width), jnp.float32), -5.0, 5.0)
    return (queries, keys)


def draw_queries(key, part):
    return paired_rows(key)[0].astype(jnp.bfloat16)


def draw_keys(key, part):
    return paired_rows(key)[1].astype(jnp.bfloat16)


def draw_cum_gate(key, part):
    key_fast, key_block, key_rough, key_index_offset, key_length = jax.random.split(jax.random.fold_in(key, 23), 5)
    fast = jax.random.randint(key_fast, (HEAD_COUNT,), 0, 2).astype(jnp.float32)
    blocks = TOKEN_COUNT // TOK_DEV
    block_factor = jnp.exp(jax.random.uniform(key_block, (blocks, 1), jnp.float32, 0.0, jnp.log(3.0)))
    block_factor = jnp.repeat(block_factor, TOK_DEV, axis=0)
    rough = jax.random.uniform(key_rough, (TOKEN_COUNT, HEAD_COUNT), jnp.float32, 0.5, 1.5)
    base = fast * (1.0 / 40.0) + (1.0 - fast) * (0.6 / TOKEN_COUNT)
    stride_offset = -base[None, :] * block_factor * rough
    group_row_block = jax.random.randint(key_index_offset, (4,), 0, TOKEN_COUNT)
    group_row_count = jnp.log(jax.random.uniform(key_length, (4, HEAD_COUNT), jnp.float32, 0.5, 0.8))
    stride_offset = stride_offset.at[group_row_block].add(group_row_count)
    return jnp.cumsum(stride_offset, axis=0)


def block_scale(key, dims, shards, least, largest):
    def one(dim, parts):
        draws = jax.random.uniform(jax.random.fold_in(jax.random.fold_in(key, 6), dim), (parts,), jnp.float32, least / len(shards), largest / len(shards))
        return jnp.repeat(jnp.exp(draws), dims[dim] // parts).reshape((-1,) + (1,) * (len(dims) - dim - 1))

    factor_of = one(*shards[0])
    for cut in shards[1:]:
        factor_of = factor_of * one(*cut)
    return factor_of


def normal_values(rng, dims, spread, limit, pieces=(), held_as=jnp.bfloat16):
    entries = jax.random.normal(rng, dims, jnp.float32) * spread
    if len(pieces) > 0:
        entries = block_scale(rng, dims, pieces, -0.22, 0.18) * entries
    return jnp.clip(entries, min=-limit, max=limit).astype(held_as)


def setup_inputs(seed: int = 0) -> dict:
    key_of = jax.random.split(jax.random.key(seed), 11)
    resid = normal_values(key_of[0], (TOKEN_COUNT, D), 1.0, 6.0, ((0, 32),))
    queries = draw_queries(jax.random.fold_in(key_of[10], 71), 0)
    keys = draw_keys(jax.random.fold_in(key_of[10], 71), 0)
    values = normal_values(key_of[3], (TOKEN_COUNT, HEAD_COUNT * HEAD_DIM), 1.0, 6.0, ((0, 8), (1, 4)))
    cum_gate = draw_cum_gate(jax.random.fold_in(key_of[10], 71), 0)
    out_weight = normal_values(key_of[5], (HEAD_COUNT * HEAD_DIM, D), (HEAD_COUNT * HEAD_DIM // 4) ** -0.5, 0.375, ((0, 4),))
    norm_gain = jnp.clip(1.0 + 0.18 * jax.random.normal(key_of[6], (D,), jnp.float32), 0.1, 1.9)
    gate_weight = normal_values(key_of[7], (D, FF), D ** -0.5, 0.125, ((0, 8), (1, 4)))
    up_weight = normal_values(key_of[8], (D, FF), D ** -0.5, 0.125, ((0, 8), (1, 4)))
    down_weight = normal_values(key_of[9], (FF, D), FF ** -0.5, 0.078125, ((0, 4), (1, 8)))
    return dict(resid=resid, queries=queries, keys=keys, values=values, cum_gate=cum_gate, out_weight=out_weight, norm_gain=norm_gain, gate_weight=gate_weight, up_weight=up_weight, down_weight=down_weight)


def reference(resid, queries, keys, values, cum_gate, out_weight, norm_gain, gate_weight, up_weight, down_weight):
    width = HEAD_COUNT * HEAD_DIM
    total_len = queries.shape[0]
    scale = HEAD_DIM ** (-0.5)
    key_heads = keys.astype(jnp.float32).reshape(total_len, HEAD_COUNT, HEAD_DIM).transpose(1, 0, 2)
    value_heads = values.astype(jnp.float32).reshape(total_len, HEAD_COUNT, HEAD_DIM).transpose(1, 0, 2)
    key_pos = jnp.arange(total_len, dtype=jnp.int32)
    gate_rows = cum_gate.T

    def block(index):
        start = (index * TOK_DEV).astype(jnp.int32)
        query_block = lax.dynamic_slice_in_dim(queries, start, TOK_DEV, 0).astype(jnp.float32)
        query_block = query_block.reshape(TOK_DEV, HEAD_COUNT, HEAD_DIM).transpose(1, 0, 2)
        gate_block = lax.dynamic_slice_in_dim(cum_gate, start, TOK_DEV, 0).T
        score = jnp.einsum('hqd,hkd->hqk', query_block, key_heads) * scale
        score = score + gate_block[:, :, None] - gate_rows[:, None, :]
        query_pos = start + jnp.arange(TOK_DEV, dtype=jnp.int32)
        score = jnp.where(key_pos[None, None, :] <= query_pos[None, :, None], score, -jnp.inf)
        top = lax.optimization_barrier(jnp.max(score, axis=-1, keepdims=True))
        weight = jnp.exp(score - top)
        total = lax.optimization_barrier(jnp.sum(weight, axis=-1, keepdims=True))
        weight_b = lax.optimization_barrier(weight.astype(jnp.bfloat16)).astype(jnp.float32)
        numer = jnp.einsum('hqk,hkd->hqd', weight_b, value_heads)
        result = (numer / total).transpose(1, 0, 2).reshape(TOK_DEV, width)
        return result.astype(jnp.bfloat16)
    attn = lax.map(block, jnp.arange(N_SP, dtype=jnp.int32)).reshape(total_len, width)
    group = width // N_TP
    proj = jnp.zeros((total_len, D), jnp.float32)
    for index in range(N_TP):
        term = jnp.dot(attn[:, index * group:(index + 1) * group], out_weight[index * group:(index + 1) * group], preferred_element_type=jnp.float32)
        proj = proj + lax.optimization_barrier(term.astype(jnp.bfloat16)).astype(jnp.float32)
    mixed = resid.astype(jnp.float32) + proj
    normed = (mixed * lax.rsqrt(lax.optimization_barrier(jnp.mean(mixed * mixed, axis=-1, keepdims=True)) + 1e-06) * norm_gain).astype(jnp.bfloat16)
    gate = jnp.dot(normed, gate_weight, preferred_element_type=jnp.float32)
    upper = jnp.dot(normed, up_weight, preferred_element_type=jnp.float32)
    hidden = (jax.nn.silu(gate) * upper).astype(jnp.bfloat16)
    hid_group = FF // N_TP
    ffn = jnp.zeros((total_len, D), jnp.float32)
    for index in range(N_TP):
        term = jnp.dot(hidden[:, index * hid_group:(index + 1) * hid_group], down_weight[index * hid_group:(index + 1) * hid_group], preferred_element_type=jnp.float32)
        ffn = ffn + lax.optimization_barrier(term.astype(jnp.bfloat16)).astype(jnp.float32)
    return (mixed + 0.5 * ffn).astype(jnp.bfloat16)
```

```python
import functools

import jax
import jax.numpy as jnp
from jax import lax
from jax.experimental import pallas as pl
from jax.experimental.pallas import tpu as pltpu
from jax.sharding import Mesh
from jax.sharding import PartitionSpec as P

HEAD_DIM = 64
LOG2E = 1.4426950408889634
AXES = ("zh", "zp", "x", "y", "c")
MESH = pl.DeviceIdType.MESH


def rms_norm(mixed, norm_gain):
    scaled = mixed * lax.rsqrt(jnp.mean(mixed * mixed, axis=-1, keepdims=True) + 1e-06) * norm_gain
    return scaled.astype(jnp.bfloat16)


def place():
    return tuple(lax.axis_index(a) for a in AXES)


def peer(z, x):
    _, _, _, y, c = place()
    return (z // 2, lax.rem(z, 2), x, y, c)


def attend(q_ref, kv_ref, g_ref, shard, x_here, rows, emit):
    half = rows // 2
    part = half // 2
    two = 2 * HEAD_DIM
    packed = q_ref[shard]
    low = lax.broadcasted_iota(jnp.int32, (part, two), 1) < HEAD_DIM
    zero = jnp.zeros_like(packed)
    queries = (
        jnp.where(low, packed, zero),
        jnp.where(low, pltpu.roll(packed, HEAD_DIM, 1), zero),
    )
    gate_own = g_ref[2 * shard + x_here]
    scale = HEAD_DIM ** (-0.5) * LOG2E
    gates = []
    for h in range(2):
        eye = lax.broadcasted_iota(jnp.int32, (part, half), 1) == (
            lax.broadcasted_iota(jnp.int32, (part, half), 0) + h * part
        )
        gates.append(jnp.sum(jnp.where(eye, gate_own, 0.0), axis=1, keepdims=True))

    def step(j, state, masked):
        best, total, numer = state
        start = pl.multiple_of(j * rows, rows)
        kv = kv_ref[pl.ds(start, rows), :]
        gate_k = jnp.concatenate([g_ref[2 * j], g_ref[2 * j + 1]], axis=1)
        new_best, new_total, new_numer = [], [], []
        for h in range(2):
            s = lax.dot_general(
                queries[h], kv, (((1,), (1,)), ((), ())), preferred_element_type=jnp.float32
            )
            s = s * scale - gate_k
            if masked:
                row = lax.broadcasted_iota(jnp.int32, s.shape, 0) + x_here * half + h * part
                col = lax.broadcasted_iota(jnp.int32, s.shape, 1)
                s = jnp.where(col <= row, s, -1e30)
            top = jnp.maximum(best[h], jnp.max(s, axis=1, keepdims=True) + gates[h])
            keep = jnp.exp2(best[h] - top)
            w = jnp.exp2(s + (gates[h] - top))
            new_best.append(top)
            new_total.append(total[h] * keep + jnp.sum(w, axis=1, keepdims=True))
            new_numer.append(
                numer[h] * keep
                + lax.dot_general(
                    w.astype(jnp.bfloat16), kv, (((1,), (0,)), ((), ())),
                    preferred_element_type=jnp.float32,
                )
            )
        return tuple(new_best), tuple(new_total), tuple(new_numer)

    column = jnp.zeros((part, 1), jnp.float32)
    block = jnp.zeros((part, two), jnp.float32)
    state = ((column - 1e30, column - 1e30), (column, column), (block, block))
    state = step(shard, state, True)
    state = lax.fori_loop(0, shard, lambda j, s: step(j, s, False), state)
    _, total, numer = state
    first = pltpu.roll(numer[0] / total[0], HEAD_DIM, 1)
    emit(jnp.where(low, first, numer[1] / total[1]).astype(jnp.bfloat16))


def front_kernel(
    rows, cut,
    q_in, kv_in, g_in, gate_in, up_in, down_in,
    o_all, gate_all, up_all, down_all,
    q_all, kv_all, g_all, o_buf,
    sem_q, sem_kv, sem_g, sem_o, sem_fw, rec_q, rec_kv, rec_g, rec_o,
    sem_w, sem_wf, rec_w, sem_own,
):
    zh, zp, x, _, _ = place()
    z = zh * 2 + zp
    along_z = q_in.shape[0]
    shards = 2 * along_z
    me = z * 2 + x
    other = 1 - x
    depth = gate_in.shape[0]
    block = down_in.shape[1]

    def remote(src, dst, send, recv, target):
        return pltpu.make_async_remote_copy(
            src_ref=src, dst_ref=dst, send_sem=send, recv_sem=recv,
            device_id=target, device_id_type=MESH,
        )

    barrier = pltpu.get_barrier_semaphore()
    for d in range(1, shards):
        t = lax.rem(me + d, shards)
        pl.semaphore_signal(barrier, inc=1, device_id=peer(t // 2, lax.rem(t, 2)), device_id_type=MESH)
    pl.semaphore_wait(barrier, shards - 1)

    def kv_rows(s):
        return kv_all.at[pl.ds(pl.multiple_of(s * rows, rows), rows)]

    def send_kv(d):
        t = lax.rem(z + d, along_z)
        return remote(kv_in.at[t], kv_rows(me), sem_kv.at[d], rec_kv.at[me], peer(t, x if d else other))

    def send_q(d):
        t = lax.rem(me + d, shards)
        tz, tx = t // 2, lax.rem(t, 2)
        return remote(q_in.at[tz, tx], q_all.at[me], sem_q.at[d], rec_q.at[me], peer(tz, tx))

    def send_g(d):
        t = lax.rem(me + d, shards)
        tz, tx = t // 2, lax.rem(t, 2)
        return remote(g_in.at[tz], g_all.at[pl.ds(2 * me, 2)], sem_g.at[d], rec_g.at[me], peer(tz, tx))

    def forward_kv(d):
        s = lax.rem(z + d, along_z) * 2 + x
        return remote(kv_rows(s), kv_rows(s), sem_fw.at[d], rec_kv.at[s], peer(z, other))

    def arrive_kv(s):
        return remote(kv_rows(s), kv_rows(s), sem_fw.at[0], rec_kv.at[s], peer(z, other))

    def piece(m, s, wide, source):
        if m < 2:
            ref_in, ref_all = (gate_in, gate_all) if m == 0 else (up_in, up_all)
            size = gate_all.shape[1] if wide else cut
            dst = ref_all.at[pl.ds(pl.multiple_of(s * depth, depth), depth), pl.ds(0, size)]
            src = ref_in.at[:, pl.ds(cut if wide else 0, size)] if source else dst
        else:
            size = down_in.shape[0] - cut if wide else cut
            dst = down_all.at[s, pl.ds(0, size), :]
            src = down_in.at[pl.ds(cut if wide else 0, size), :] if source else dst
        return src, dst

    def send_w(m, d, act):
        t = lax.rem(z + d, along_z)
        target = peer(t, x if d else other)
        for wide in (False, True):
            def go(wide=wide):
                src, dst = piece(m, me, wide, True)
                getattr(remote(src, dst, sem_w.at[m, d], rec_w.at[m, me], target), act)()

            pl.when(lax.rem(t, 2) == int(wide))(go)

    def forward_w(m, d, act):
        s = lax.rem(z + d, along_z) * 2 + x
        for wide in (False, True):
            def go(wide=wide):
                src, dst = piece(m, s, wide, False)
                cp = remote(src, dst, sem_wf.at[m, d], rec_w.at[m, s], peer(z, other))
                getattr(cp, act)()

            pl.when(zp == int(wide))(go)

    def arrive_w(m, s):
        for wide in (False, True):
            def go(wide=wide):
                src, dst = piece(m, s, wide, False)
                remote(src, dst, sem_wf.at[m, 0], rec_w.at[m, s], peer(z, other)).wait_recv()

            pl.when(zp == int(wide))(go)

    for d in range(1, along_z):
        send_kv(d).start()
    send_kv(0).start()
    for d in range(1, shards):
        send_g(d).start()
        send_q(d).start()
    for d in range(along_z):
        send_w(0, d, "start")
    send_w(1, 0, "start")
    for wide in (False, True):
        def keep(wide=wide):
            for m in range(3):
                src, dst = piece(m, me, wide, True)
                pltpu.make_async_copy(src, dst, sem_own.at[m]).start()
            size = down_in.shape[0] - cut if wide else cut
            tail = down_all.shape[1] - size
            for s in range(shards):
                down_all[s, pl.ds(size, tail), :] = jnp.zeros((tail, block), down_all.dtype)

        pl.when(zp == int(wide))(keep)
    q_all[me] = q_in[z, x]
    kv_all[pl.ds(pl.multiple_of(me * rows, rows), rows), :] = kv_in[z]
    for k in range(2):
        g_all[2 * me + k] = g_in[z, k]
    for d in range(1, along_z):
        s = lax.rem(z + d, along_z) * 2 + x
        arrive_kv(s).wait_recv()
        forward_kv(d).start()
    for d in range(1, shards):
        s = lax.rem(me + d, shards)
        sz, sx = s // 2, lax.rem(s, 2)
        remote(q_all.at[s], q_all.at[s], sem_q.at[d], rec_q.at[s], peer(sz, sx)).wait_recv()
        remote(g_in.at[z], g_all.at[pl.ds(2 * s, 2)], sem_g.at[d], rec_g.at[s], peer(sz, sx)).wait_recv()
    for d in range(along_z):
        arrive_kv(lax.rem(z + d, along_z) * 2 + other).wait_recv()

    def send_o(s):
        return remote(o_buf.at[s], o_all.at[me], sem_o.at[s], rec_o.at[me], peer(s // 2, lax.rem(s, 2)))

    def chunk(s, _):
        def emit(value):
            o_buf[s] = value

            @pl.when(s != me)
            def _():
                send_o(s).start()

            @pl.when(s == me)
            def _():
                o_all[me] = value

        attend(q_all, kv_all, g_all, s, x, rows, emit)

        @pl.when(s == shards // 2)
        def _():
            for d in range(1, along_z):
                send_w(1, d, "start")

        return 0

    lax.fori_loop(0, shards, chunk, 0)
    for m in range(3):
        if m == 2:
            for d in range(along_z):
                send_w(m, d, "start")
        for d in range(1, along_z):
            arrive_w(m, lax.rem(z + d, along_z) * 2 + x)
            forward_w(m, d, "start")
    for wide in (False, True):
        def kept(wide=wide):
            for m in range(3):
                src, dst = piece(m, me, wide, True)
                pltpu.make_async_copy(src, dst, sem_own.at[m]).wait()

        pl.when(zp == int(wide))(kept)
    for m in range(3):
        for d in range(along_z):
            arrive_w(m, lax.rem(z + d, along_z) * 2 + other)
        for d in range(along_z):
            send_w(m, d, "wait_send")
        for d in range(1, along_z):
            forward_w(m, d, "wait_send")
    for d in range(1, shards):
        s = lax.rem(me + d, shards)
        remote(o_buf.at[s], o_all.at[s], sem_o.at[s], rec_o.at[s], peer(s // 2, lax.rem(s, 2))).wait()
        send_g(d).wait_send()
        send_q(d).wait_send()
    for d in range(along_z):
        send_kv(d).wait_send()
    for d in range(1, along_z):
        forward_kv(d).wait_send()


def front(queries, keys, values, cum_gate, gate_weight, up_weight, down_weight, cut):
    rows, _ = queries.shape
    heads = cum_gate.shape[1]
    along_z = heads
    shards = 2 * along_z
    two = 2 * HEAD_DIM
    part = rows // 4
    kv = jnp.concatenate(
        [keys.reshape(rows, heads, HEAD_DIM), values.reshape(rows, heads, HEAD_DIM)], axis=2
    ).transpose(1, 0, 2)
    q = queries.reshape(2, 2, part, heads, HEAD_DIM).transpose(3, 0, 2, 1, 4)
    q = q.reshape(heads, 2, part, two)
    g = (cum_gate.T * LOG2E).reshape(heads, 2, 1, rows // 2)
    depth, hidden = gate_weight.shape
    pad = -hidden % 128
    gate_weight = jnp.pad(gate_weight, ((0, 0), (0, pad)))
    up_weight = jnp.pad(up_weight, ((0, 0), (0, pad)))
    wide = hidden + pad - cut
    vmem = pl.BlockSpec(memory_space=pltpu.VMEM)
    hbm = pl.BlockSpec(memory_space=pl.ANY)
    dma = pltpu.SemaphoreType.DMA
    bf16 = jnp.bfloat16
    return pl.pallas_call(
        functools.partial(front_kernel, rows, cut),
        in_specs=[vmem, vmem, vmem, hbm, hbm, hbm],
        out_specs=[vmem] * 4,
        out_shape=[
            jax.ShapeDtypeStruct((shards, part, two), bf16),
            jax.ShapeDtypeStruct((shards * depth, wide), bf16),
            jax.ShapeDtypeStruct((shards * depth, wide), bf16),
            jax.ShapeDtypeStruct((shards, wide, down_weight.shape[1]), bf16),
        ],
        scratch_shapes=[
            pltpu.VMEM((shards, part, two), bf16),
            pltpu.VMEM((shards * rows, two), bf16),
            pltpu.VMEM((2 * shards, 1, rows // 2), jnp.float32),
            pltpu.VMEM((shards, part, two), bf16),
            dma((shards,)), dma((along_z,)), dma((shards,)), dma((shards,)), dma((along_z,)),
            dma((shards,)), dma((shards,)), dma((shards,)), dma((shards,)),
            dma((3, along_z)), dma((3, along_z)), dma((3, shards)), dma((3,)),
        ],
        compiler_params=pltpu.CompilerParams(
            collective_id=0, has_side_effects=True, vmem_limit_bytes=56 * 2**20
        ),
    )(q, kv, g, gate_weight, up_weight, down_weight)


def fast(
    cut, resid, queries, keys, values, cum_gate, out_weight, norm_gain, gate_weight, up_weight, down_weight
):
    rows, width = queries.shape
    heads = cum_gate.shape[1]
    hidden = gate_weight.shape[1]
    part = rows // 4
    o_all, gate_all, up_all, down_all = front(
        queries, keys, values, cum_gate, gate_weight, up_weight, down_weight, cut
    )
    attn = o_all.reshape(heads, 2, part, 2, HEAD_DIM).transpose(1, 3, 2, 0, 4).reshape(rows, width)
    out_full = lax.all_gather(out_weight, ("y", "c"), axis=0, tiled=True)
    own_rows = lax.all_to_all(attn, ("y", "c"), split_axis=0, concat_axis=1, tiled=True)
    mixed = resid.astype(jnp.float32) + jnp.dot(
        own_rows, out_full, preferred_element_type=jnp.float32
    )
    normed = rms_norm(mixed, norm_gain)
    normed_all = lax.all_gather(normed, ("zp", "y", "c"), axis=0, tiled=True)
    gate_sum = jnp.dot(normed_all, gate_all, preferred_element_type=jnp.float32)
    up_sum = jnp.dot(normed_all, up_all, preferred_element_type=jnp.float32)
    count = jnp.where(lax.axis_index("zp") == 0, cut, hidden - cut)
    lane = lax.broadcasted_iota(jnp.int32, gate_sum.shape, 1)
    hid = jnp.where(lane < count, jax.nn.silu(gate_sum) * up_sum, 0.0).astype(jnp.bfloat16)
    parts = [
        jnp.dot(hid, down_all[s], preferred_element_type=jnp.float32).astype(jnp.bfloat16)
        for s in range(down_all.shape[0])
    ]
    ffn = lax.psum_scatter(
        jnp.concatenate(parts, axis=1), ("zp", "y", "c"), scatter_dimension=0, tiled=True
    )
    return (mixed + 0.5 * ffn.astype(jnp.float32)).astype(jnp.bfloat16)


def rounded(term):
    return term.astype(jnp.bfloat16).astype(jnp.float32)


def flash_kernel(rows, q_block, shard_ref, q_ref, k_ref, v_ref, gate_q_ref, gate_k_ref, out_ref):
    pair = pl.program_id(0)
    block = pl.program_id(1)
    shard = shard_ref[0]
    q = q_ref[...]
    lane = lax.broadcasted_iota(jnp.int32, (q_block, 2 * HEAD_DIM), 1)
    low = lane < HEAD_DIM
    zero = jnp.zeros_like(q)
    q_heads = (jnp.where(low, q, zero), jnp.where(low, zero, q))
    gate_q = gate_q_ref[...]
    gate_lane = lax.broadcasted_iota(jnp.int32, gate_q.shape, 1)
    gates = tuple(
        jnp.sum(jnp.where(gate_lane == 2 * pair + h, gate_q, 0.0), axis=1, keepdims=True) * LOG2E
        for h in range(2)
    )
    scale = HEAD_DIM ** (-0.5) * LOG2E

    def step(j, state, masked):
        best, total, numer = state
        start = pl.multiple_of(j * rows, rows)
        k = k_ref[pl.ds(start, rows), :]
        v = v_ref[pl.ds(start, rows), :]
        new_best, new_total, parts, decay = [], [], [], []
        for h in range(2):
            s = lax.dot_general(
                q_heads[h], k, (((1,), (1,)), ((), ())), preferred_element_type=jnp.float32
            )
            gate_k = gate_k_ref[j, 0, h : h + 1, :] * LOG2E
            s = s * scale + (gates[h] - gate_k)
            if masked:
                row = lax.broadcasted_iota(jnp.int32, s.shape, 0) + block * q_block
                col = lax.broadcasted_iota(jnp.int32, s.shape, 1)
                s = jnp.where(col <= row, s, -1e30)
            top = jnp.maximum(best[h], jnp.max(s, axis=1, keepdims=True))
            keep = jnp.exp2(best[h] - top)
            w = jnp.exp2(s - top)
            new_best.append(top)
            new_total.append(total[h] * keep + jnp.sum(w, axis=1, keepdims=True))
            parts.append(
                lax.dot_general(
                    w.astype(jnp.bfloat16), v, (((1,), (0,)), ((), ())),
                    preferred_element_type=jnp.float32,
                )
            )
            decay.append(keep)
        numer = numer * jnp.where(low, decay[0], decay[1]) + jnp.where(low, parts[0], parts[1])
        return tuple(new_best), tuple(new_total), numer

    column = jnp.zeros((q_block, 1), jnp.float32)
    state = (
        (column - 1e30, column - 1e30),
        (column, column),
        jnp.zeros((q_block, 2 * HEAD_DIM), jnp.float32),
    )
    state = step(shard, state, True)
    state = lax.fori_loop(0, shard, lambda j, s: step(j, s, False), state)
    _, total, numer = state
    out_ref[...] = (numer / jnp.where(low, total[0], total[1])).astype(jnp.bfloat16)


def flash(shard, queries, kv_all, cum_gate, gates_all):
    rows, width = queries.shape
    pairs = width // (2 * HEAD_DIM)
    count = kv_all.shape[0]
    shards = count // rows
    heads = cum_gate.shape[1]
    q_block = 256 if rows % 256 == 0 else rows
    two = 2 * HEAD_DIM
    gates_all = gates_all.reshape(shards, pairs, 2, rows)
    return pl.pallas_call(
        functools.partial(flash_kernel, rows, q_block),
        grid=(pairs, rows // q_block),
        in_specs=[
            pl.BlockSpec(memory_space=pltpu.SMEM),
            pl.BlockSpec((q_block, two), lambda p, i: (i, p)),
            pl.BlockSpec((count, two), lambda p, i: (0, p)),
            pl.BlockSpec((count, two), lambda p, i: (0, pairs + p)),
            pl.BlockSpec((q_block, heads), lambda p, i: (i, 0)),
            pl.BlockSpec((shards, 1, 2, rows), lambda p, i: (0, p, 0, 0)),
        ],
        out_specs=pl.BlockSpec((q_block, two), lambda p, i: (i, p)),
        out_shape=jax.ShapeDtypeStruct((rows, width), jnp.bfloat16),
        compiler_params=pltpu.CompilerParams(vmem_limit_bytes=40 * 2**20),
        cost_estimate=pl.CostEstimate(
            flops=8 * rows * count * width,
            bytes_accessed=4 * count * width,
            transcendentals=rows * count * width // HEAD_DIM,
        ),
    )(shard.reshape(1), queries, kv_all, kv_all, cum_gate, gates_all)


def shift(value, axis, size, step):
    return lax.ppermute(value, axis, [(i, (i + step) % size) for i in range(size)])


def exchange(weight, split, joined, size):
    here = lax.axis_index("x")
    width = weight.shape[split] // size
    pieces = []
    for step in range(size):
        target = lax.rem(here + step, size)
        piece = lax.dynamic_slice_in_dim(weight, target * width, width, split)
        pieces.append(piece if step == 0 else shift(piece, "x", size, step))
    if size == 1:
        return pieces[0]
    if size == 2:
        first = here == 0
        return jnp.concatenate(
            [jnp.where(first, pieces[0], pieces[1]), jnp.where(first, pieces[1], pieces[0])], joined
        )
    length = weight.shape[joined]
    shape = list(pieces[0].shape)
    shape[joined] = length * size
    whole = jnp.zeros(shape, weight.dtype)
    for step in range(size):
        source = lax.rem(here - step + size, size)
        whole = lax.dynamic_update_slice_in_dim(whole, pieces[step], source * length, joined)
    return whole


def local(
    resid,
    queries,
    keys,
    values,
    cum_gate,
    out_weight,
    norm_gain,
    gate_weight,
    up_weight,
    down_weight,
):
    along_x = lax.axis_size("x")
    groups = lax.axis_size("tp")
    shard = lax.axis_index("z") * along_x + lax.axis_index("x")
    gates_all = lax.all_gather(cum_gate.T, ("z", "x"), axis=0)
    kv_all = lax.all_gather(jnp.concatenate([keys, values], axis=1), ("z", "x"), axis=0, tiled=True)
    proj_weights = [out_weight] + [shift(out_weight, "tp", groups, d) for d in range(1, groups)]
    gate_cols = exchange(gate_weight, 1, 0, along_x)
    up_cols = exchange(up_weight, 1, 0, along_x)
    down_rows = exchange(down_weight, 0, 1, along_x)
    along_z = lax.axis_size("z")
    gate_full = lax.all_gather(gate_cols, "z", axis=0, tiled=True)
    up_full = lax.all_gather(up_cols, "z", axis=0, tiled=True)
    down_parts = [down_rows] + [shift(down_rows, "z", along_z, d) for d in range(1, along_z)]

    queries, gate_cols, up_cols, down_rows = lax.optimization_barrier(
        (queries, gate_cols, up_cols, down_rows)
    )
    attn = flash(shard.astype(jnp.int32), queries, kv_all, cum_gate, gates_all)

    own_rows = lax.all_to_all(attn, "tp", split_axis=0, concat_axis=1, tiled=True)
    width = attn.shape[1]
    here = lax.axis_index("tp")
    mixed = resid.astype(jnp.float32)
    for d in range(groups):
        group = lax.rem(here - d + groups, groups)
        part = lax.dynamic_slice_in_dim(own_rows, group * width, width, 1)
        mixed = mixed + rounded(
            jnp.dot(part, proj_weights[d], preferred_element_type=jnp.float32)
        )
    normed, up_full = lax.optimization_barrier((rms_norm(mixed, norm_gain), up_full))
    normed_all = lax.all_gather(normed, ("x", "tp"), axis=0, tiled=True)
    gate_sum = jnp.dot(normed_all, gate_full, preferred_element_type=jnp.float32)
    up_sum = jnp.dot(normed_all, up_full, preferred_element_type=jnp.float32)
    hidden = (jax.nn.silu(gate_sum) * up_sum).astype(jnp.bfloat16)
    ffn_part = jnp.concatenate(
        [
            jnp.dot(hidden, part, preferred_element_type=jnp.float32).astype(jnp.bfloat16)
            for part in down_parts
        ],
        axis=1,
    )
    turned = lax.psum_scatter(ffn_part, ("x", "tp"), scatter_dimension=0, tiled=True)
    block = down_parts[0].shape[1]
    ffn = jnp.concatenate(
        [
            lax.dynamic_slice_in_dim(
                turned, lax.rem(lax.axis_index("z") - c + along_z, along_z) * block, block, 1
            )
            for c in range(along_z)
        ],
        axis=1,
    ).astype(jnp.float32)
    return (mixed + 0.5 * ffn).astype(jnp.bfloat16)


def general(mesh):
    along_sp = mesh.shape["sp"]
    along_x = 2 if along_sp % 2 == 0 else 1
    grid = Mesh(
        mesh.devices.reshape(along_sp // along_x, along_x, mesh.shape["tp"]), ("z", "x", "tp")
    )
    sp = ("z", "x")
    in_specs = (
        P(("z", "x", "tp"), None),
        P(sp, "tp"),
        P(sp, "tp"),
        P(sp, "tp"),
        P(sp, "tp"),
        P("tp", None),
        P(),
        P(sp, "tp"),
        P(sp, "tp"),
        P("tp", sp),
    )
    out_specs = P(("z", "x", "tp"), None)

    return jax.shard_map(local, mesh=grid, in_specs=in_specs, out_specs=out_specs, check_vma=False)


def solution(mesh):
    along_sp, along_tp = mesh.shape["sp"], mesh.shape["tp"]
    slow = general(mesh)

    def run(*args):
        heads = args[4].shape[1] // along_tp
        rows = args[1].shape[0] // along_sp
        hidden = args[7].shape[1] // along_tp
        cut = hidden // 2 // 128 * 128
        if along_sp != 2 * heads or heads % 2 or along_tp % 2 or rows % 128 or cut == 0:
            return slow(*args)
        grid = Mesh(mesh.devices.reshape(heads // 2, 2, 2, along_tp // 2, 2), AXES)
        sp, tp = ("zh", "zp", "x"), ("y", "c")
        in_specs = (
            P(sp + tp, None),
            P(sp, tp), P(sp, tp), P(sp, tp), P(sp, tp),
            P(tp, None),
            P(),
            P(sp, tp), P(sp, tp), P(tp, sp),
        )
        step = jax.shard_map(
            functools.partial(fast, cut), mesh=grid, in_specs=in_specs,
            out_specs=P(sp + tp, None), check_vma=False,
        )
        return step(*args)

    return run
```

```python
import functools

import jax
import jax.numpy as jnp
from jax import lax
from jax.experimental import pallas as pl
from jax.experimental.pallas import tpu as pltpu
from jax.sharding import Mesh
from jax.sharding import PartitionSpec as P

HEAD_DIM = 64
LOG2E = 1.4426950408889634
AXES = ("zh", "zp", "x", "y", "c")
MESH = pl.DeviceIdType.MESH


def rms_norm(mixed, norm_gain):
    scaled = mixed * lax.rsqrt(jnp.mean(mixed * mixed, axis=-1, keepdims=True) + 1e-06) * norm_gain
    return scaled.astype(jnp.bfloat16)


def place():
    return tuple(lax.axis_index(a) for a in AXES)


def swap(value):
    return pltpu.roll(value, HEAD_DIM, 1)


def attend(buf, g_row, shard, x_here, rows, q_start, emit):
    half = rows // 2
    part = half // 2
    two = 2 * HEAD_DIM
    packed = buf[shard, pl.ds(q_start, part), :]
    low = lax.broadcasted_iota(jnp.int32, (part, two), 1) < HEAD_DIM
    zero = jnp.zeros_like(packed)
    queries = (jnp.where(low, packed, zero), jnp.where(low, swap(packed), zero))
    gate_own = g_row[shard, :, pl.ds(pl.multiple_of(x_here * half, 128), half)]
    scale = HEAD_DIM ** (-0.5) * LOG2E
    gates = []
    for h in range(2):
        eye = lax.broadcasted_iota(jnp.int32, (part, half), 1) == (
            lax.broadcasted_iota(jnp.int32, (part, half), 0) + h * part
        )
        gates.append(jnp.sum(jnp.where(eye, gate_own, 0.0), axis=1, keepdims=True))

    def step(j, state, masked):
        best, total, numer = state
        kv = buf[j, pl.ds(0, rows), :]
        gate_k = g_row[j]
        new_best, new_total, new_numer = [], [], []
        for h in range(2):
            s = lax.dot_general(
                queries[h], kv, (((1,), (1,)), ((), ())), preferred_element_type=jnp.float32
            )
            s = s * scale - gate_k
            if masked:
                row = lax.broadcasted_iota(jnp.int32, s.shape, 0) + x_here * half + h * part
                col = lax.broadcasted_iota(jnp.int32, s.shape, 1)
                s = jnp.where(col <= row, s, -1e30)
            top = jnp.maximum(best[h], jnp.max(s, axis=1, keepdims=True) + gates[h])
            keep = jnp.exp2(best[h] - top)
            w = jnp.exp2(s + (gates[h] - top))
            new_best.append(top)
            new_total.append(total[h] * keep + jnp.sum(w, axis=1, keepdims=True))
            new_numer.append(
                numer[h] * keep
                + lax.dot_general(
                    w.astype(jnp.bfloat16), kv, (((1,), (0,)), ((), ())),
                    preferred_element_type=jnp.float32,
                )
            )
        return tuple(new_best), tuple(new_total), tuple(new_numer)

    column = jnp.zeros((part, 1), jnp.float32)
    block = jnp.zeros((part, two), jnp.float32)
    state = ((column - 1e30, column - 1e30), (column, column), (block, block))
    state = step(shard, state, True)
    state = lax.fori_loop(0, shard, lambda j, s: step(j, s, False), state)
    _, total, numer = state
    first = swap(numer[0] / total[0])
    emit(jnp.where(low, first, numer[1] / total[1]).astype(jnp.bfloat16))


def layer_kernel(
    cut,
    resid_in, q_in, k_in, v_in, g_in, gain_in, out_in, gate_in, up_in, down_in,
    result,
    snd, buf, g_row, o_buf, o_all, a_buf, a_all, out_all, gate_all, up_all, down_all,
    mixed, normed, hid, part_buf, r0, s1, r1, s2, r2,
    sem_x, rec_kv, rec_q, sem_o, rec_o, sem_a, rec_a, sem_ow, rec_ow,
    sem_w, sem_wf, rec_w, sem_own, sem_ag, rec_ag, rec_agp, sem_r, rec_r,
):
    zh, zp, x, y, c = place()
    z = zh * 2 + zp
    rows, width = q_in.shape
    along_z = g_in.shape[0]
    shards = 2 * along_z
    groups = out_all.shape[0]
    me = z * 2 + x
    other = 1 - x
    tp = y * 2 + c
    depth, hidden = gate_in.shape
    block = down_in.shape[1]
    part = rows // 4
    f32, bf16 = jnp.float32, jnp.bfloat16
    two = 2 * HEAD_DIM
    kv_end = rows + 48
    q_end = kv_end + part
    lanes = g_in.shape[1]

    def sp_peer(zz, xx):
        return (zz // 2, lax.rem(zz, 2), xx, y, c)

    def tp_peer(t):
        return (zh, zp, x, t // 2, lax.rem(t, 2))

    partner = (zh, zp, x, y, 1 - c)
    y_peer = (zh, zp, x, 1 - y, c)
    z_peer = (zh, 1 - zp, x, y, c)

    def remote(src, dst, send, recv, target):
        return pltpu.make_async_remote_copy(
            src_ref=src, dst_ref=dst, send_sem=send, recv_sem=recv,
            device_id=target, device_id_type=MESH,
        )

    barrier = pltpu.get_barrier_semaphore()
    for d in range(1, shards):
        t = lax.rem(me + d, shards)
        pl.semaphore_signal(
            barrier, inc=1, device_id=sp_peer(t // 2, lax.rem(t, 2)), device_id_type=MESH
        )
    for d in range(1, groups):
        pl.semaphore_signal(
            barrier, inc=1, device_id=tp_peer(lax.rem(tp + d, groups)), device_id_type=MESH
        )

    low = lax.broadcasted_iota(jnp.int32, (rows, two), 1) < HEAD_DIM
    low_q = lax.broadcasted_iota(jnp.int32, (part, two), 1) < HEAD_DIM
    for h in range(along_z):
        pair = slice(h // 2 * two, (h // 2 + 1) * two)
        k2, v2 = k_in[:, pair], v_in[:, pair]
        snd[h, 0:rows, :] = jnp.where(low, k2 if h % 2 == 0 else swap(k2), swap(v2) if h % 2 == 0 else v2)
        rest = g_in[h]
        pad = jnp.zeros((16 - lanes, 128), bf16)
        for k in range(3):
            piece = rest.astype(bf16)
            rest = rest - piece.astype(f32)
            snd[h, rows + 16 * k : rows + 16 * (k + 1), :] = jnp.concatenate([piece, pad], axis=0)
        for xd in range(2):
            qa = q_in[xd * 2 * part : (xd * 2 + 1) * part, pair]
            qb = q_in[(xd * 2 + 1) * part : (xd * 2 + 2) * part, pair]
            packed = jnp.where(low_q, qa if h % 2 == 0 else swap(qa), swap(qb) if h % 2 == 0 else qb)
            start = pl.multiple_of(kv_end + part * lax.rem(xd + x, 2), 16)
            snd[h, pl.ds(start, part), :] = packed

    pl.semaphore_wait(barrier, shards + groups - 2)

    NEAR = tuple(k * sign for k in range(1, along_z) for sign in (1, -1))

    def at_z(k, action):
        t = z + k
        pl.when((t >= 0) & (t < along_z))(lambda: action(jnp.clip(t, 0, along_z - 1)))

    def lane_x(t, act):
        cp = remote(
            snd.at[t, pl.ds(0, q_end)], buf.at[me, pl.ds(0, q_end)],
            sem_x.at[0, t], rec_kv.at[me], sp_peer(t, x),
        )
        getattr(cp, act)()

    def cross_x(t, act):
        cp = remote(
            snd.at[t, pl.ds(q_end, part)], buf.at[me, pl.ds(kv_end, part)],
            sem_x.at[1, t], rec_q.at[me], sp_peer(t, other),
        )
        getattr(cp, act)()

    def side_x(act):
        cp = remote(
            snd.at[z, pl.ds(0, kv_end)], buf.at[me, pl.ds(0, kv_end)],
            sem_x.at[2, z], rec_kv.at[me], sp_peer(z, other),
        )
        getattr(cp, act)()

    def pass_x(t, act):
        s = t * 2 + x
        cp = remote(
            buf.at[s, pl.ds(0, kv_end)], buf.at[s, pl.ds(0, kv_end)],
            sem_x.at[2, t], rec_kv.at[s], sp_peer(z, other),
        )
        getattr(cp, act)()

    for k in NEAR:
        at_z(k, lambda t: lane_x(t, "start"))
    side_x("start")
    cross_x(z, "start")
    for k in NEAR:
        at_z(k, lambda t: cross_x(t, "start"))

    pieces = 6

    def piece(p, s, wide, source):
        m, k = p // 2, p % 2
        if m < 2:
            ref_in, ref_all = (gate_in, gate_all) if m == 0 else (up_in, up_all)
            size = hidden - cut if wide else cut
            step = depth // 2
            dst = ref_all.at[
                pl.ds(pl.multiple_of(s * depth + k * step, step), step), pl.ds(0, size)
            ]
            src = ref_in.at[pl.ds(k * step, step), pl.ds(cut if wide else 0, size)] if source else dst
        else:
            size = hidden - cut if wide else cut
            step = size // 2
            dst = down_all.at[s, pl.ds(k * step, step), :]
            src = down_in.at[pl.ds((cut if wide else 0) + k * step, step), :] if source else dst
        return src, dst

    def by_width(which, action):
        for wide in (False, True):
            pl.when(which == int(wide))(functools.partial(action, wide))

    def side_w(p, act):
        def go(wide):
            src, dst = piece(p, me, wide, True)
            cp = remote(src, dst, sem_w.at[p, z], rec_w.at[p, me], sp_peer(z, other))
            getattr(cp, act)()

        by_width(zp, go)

    def send_w(p, act):
        for k in NEAR:
            def go_all(t):
                def go(wide):
                    src, dst = piece(p, me, wide, True)
                    cp = remote(src, dst, sem_w.at[p, t], rec_w.at[p, me], sp_peer(t, x))
                    getattr(cp, act)()

                by_width(lax.rem(t, 2), go)

            at_z(k, go_all)

    def pass_w(p, act):
        for k in NEAR:
            def go_all(t):
                s = t * 2 + x

                def go(wide):
                    src, dst = piece(p, s, wide, False)
                    cp = remote(src, dst, sem_wf.at[p, t], rec_w.at[p, s], sp_peer(z, other))
                    if act == "start":
                        cp.wait_recv()
                    getattr(cp, act)()

                by_width(zp, go)

            at_z(k, go_all)

    def arrive_w(p, t):
        s = t * 2 + other

        def go(wide):
            src, dst = piece(p, s, wide, False)
            remote(src, dst, sem_wf.at[p, 0], rec_w.at[p, s], sp_peer(z, other)).wait_recv()

        by_width(zp, go)

    def own_w(act):
        def go(wide):
            for p in range(pieces):
                src, dst = piece(p, me, wide, True)
                getattr(pltpu.make_async_copy(src, dst, sem_own.at[p]), act)()
            if act == "start":
                size = hidden - cut if wide else cut
                tail = down_all.shape[1] - size
                if tail:
                    for s in range(shards):
                        down_all[s, size : size + tail, :] = jnp.zeros((tail, block), bf16)

        by_width(zp, go)

    def send_out(d, act):
        t = lax.rem(tp + d, groups)
        cp = remote(out_in, out_all.at[tp], sem_ow.at[d], rec_ow.at[tp], tp_peer(t))
        getattr(cp, act)()

    send_w(0, "start")
    for d in range(1, groups):
        send_out(d, "start")
    own_w("start")
    own_out = pltpu.make_async_copy(out_in, out_all.at[tp], sem_ow.at[0])
    own_out.start()
    buf[me, 0:q_end, :] = snd[z, 0:q_end, :]

    for k in NEAR:
        def relay(t):
            s = t * 2 + x
            remote(
                snd.at[t, pl.ds(0, q_end)], buf.at[s, pl.ds(0, q_end)],
                sem_x.at[0, t], rec_kv.at[s], sp_peer(t, x),
            ).wait_recv()
            pass_x(t, "start")

        at_z(k, relay)
    for p in range(2):
        side_w(p, "start")
    for t in range(along_z):
        s = t * 2 + other
        remote(
            buf.at[s, pl.ds(0, kv_end)], buf.at[s, pl.ds(0, kv_end)],
            sem_x.at[2, 0], rec_kv.at[s], sp_peer(z, other),
        ).wait_recv()
        remote(
            snd.at[t, pl.ds(q_end, part)], buf.at[s, pl.ds(kv_end, part)],
            sem_x.at[1, t], rec_q.at[s], sp_peer(z, other),
        ).wait_recv()

    def unpack(s, _):
        g = buf[s, rows : rows + 48, :].astype(f32)
        g = g[0:16] + g[16:32] + g[32:48]
        g_row[s] = jnp.concatenate([g[k : k + 1, :] for k in range(lanes)], axis=1)
        return 0

    lax.fori_loop(0, shards, unpack, 0)

    def send_o(s):
        return remote(
            o_buf.at[s], o_all.at[me], sem_o.at[s], rec_o.at[me], sp_peer(s // 2, lax.rem(s, 2))
        )

    def chunk(s, _):
        def emit(value):
            o_buf[s] = value

            @pl.when(s != me)
            def _():
                send_o(s).start()

            @pl.when(s == me)
            def _():
                o_all[me] = value

        attend(buf, g_row, s, x, rows, kv_end, emit)

        @pl.when(s == shards // 2 - 1)
        def _():
            send_w(1, "start")

        @pl.when(s == shards - 3)
        def _():
            pass_w(0, "start")
            for p in range(2, 4):
                side_w(p, "start")
            send_w(2, "start")

        return 0

    lax.fori_loop(0, shards, chunk, 0)
    pass_w(1, "start")
    for d in range(1, shards):
        s = lax.rem(me + d, shards)
        remote(
            o_buf.at[s], o_all.at[s], sem_o.at[s], rec_o.at[s], sp_peer(s // 2, lax.rem(s, 2))
        ).wait_recv()

    for t in range(groups):
        xh, half = t // 2, t % 2
        cols = []
        for h in range(0, along_z, 2):
            a, b = o_all[2 * h + xh], o_all[2 * (h + 1) + xh]
            cols.append(
                jnp.where(low_q, a, swap(b)) if half == 0 else jnp.where(low_q, swap(a), b)
            )
        a_buf[t] = jnp.concatenate(cols, axis=1)

    def send_a(d, act):
        t = lax.rem(tp + d, groups)
        getattr(remote(a_buf.at[t], a_all.at[tp], sem_a.at[d], rec_a.at[tp], tp_peer(t)), act)()

    for d in range(1, groups):
        send_a(d, "start")
    a_all[tp] = a_buf[tp]
    send_w(3, "start")
    own_out.wait()
    for d in range(1, groups):
        t = lax.rem(tp + d, groups)
        remote(out_in, out_all.at[t], sem_ow.at[d], rec_ow.at[t], tp_peer(t)).wait_recv()
    pass_w(2, "start")
    for d in range(1, groups):
        t = lax.rem(tp + d, groups)
        remote(a_buf.at[t], a_all.at[t], sem_a.at[d], rec_a.at[t], tp_peer(t)).wait_recv()

    own_rows, model = resid_in.shape
    attn = jnp.concatenate([a_all[t] for t in range(groups)], axis=1)
    total = jnp.zeros((own_rows, 1), f32)
    stripe = 512
    for n in range(0, model, stripe):
        w = out_all[:, :, n : n + stripe].reshape(groups * width, stripe)
        value = resid_in[:, n : n + stripe].astype(f32) + jnp.dot(attn, w, preferred_element_type=f32)
        mixed[:, n : n + stripe] = value
        total = total + jnp.sum(value * value, axis=1, keepdims=True)
    factor = lax.rsqrt(total / model + 1e-6)
    chip = zp * 2 + y
    slot = chip * 2 + c
    for n in range(0, model, stripe):
        normed[slot, :, n : n + stripe] = (
            mixed[:, n : n + stripe] * factor * gain_in[:, n : n + stripe]
        ).astype(bf16)

    mid = own_rows // 2
    y_slot = (zp * 2 + 1 - y) * 2 + c
    z_slot = ((1 - zp) * 2 + y) * 2 + c
    d_slot = ((1 - zp) * 2 + 1 - y) * 2 + c

    def rows_of(s, h):
        return normed.at[s, pl.ds(h * mid, mid)]

    def ag(s, h, k, target):
        return remote(rows_of(s, h), rows_of(s, h), sem_ag.at[k], rec_ag.at[s, h], target)

    def agp(s, k):
        return remote(normed.at[s], normed.at[s], sem_ag.at[k], rec_agp.at[s], partner)

    sends = [
        agp(slot, 0), ag(slot, 0, 1, y_peer), ag(slot, 1, 2, z_peer),
        ag(slot, 1, 3, y_peer), ag(slot, 0, 4, z_peer),
    ]
    for cp in sends:
        cp.start()
    send_w(4, "start")
    send_w(5, "start")
    for p in range(4, 6):
        side_w(p, "start")
    pass_w(3, "start")

    def got(s, h):
        ag(s, h, 0, y_peer).wait_recv()

    def forward(cp):
        cp.start()
        sends.append(cp)

    got(y_slot, 0)
    forward(ag(y_slot, 0, 5, z_peer))
    got(z_slot, 1)
    forward(ag(z_slot, 1, 6, y_peer))
    own_w("wait")
    for p in range(4):
        for t in range(along_z):
            arrive_w(p, t)

    count = jnp.where(zp == 0, cut, hidden - cut)

    def expand(q):
        rows_q = normed[pl.ds(2 * q, 2)].reshape(2 * own_rows, model)
        gate = jnp.dot(rows_q, gate_all[...], preferred_element_type=f32)
        up = jnp.dot(rows_q, up_all[...], preferred_element_type=f32)
        value = gate / (1.0 + jnp.exp(-gate)) * up
        lane = lax.broadcasted_iota(jnp.int32, value.shape, 1)
        hid[q] = jnp.where(lane < count, value, 0.0).astype(bf16)

    def flip(s):
        return s + 1 - 2 * c

    agp(flip(slot), 0).wait_recv()
    expand(chip)
    got(y_slot, 1)
    forward(agp(y_slot, 7))
    got(z_slot, 0)
    forward(agp(z_slot, 8))
    agp(flip(y_slot), 0).wait_recv()
    expand(zp * 2 + 1 - y)
    agp(flip(z_slot), 0).wait_recv()
    expand((1 - zp) * 2 + y)
    got(d_slot, 0)
    got(d_slot, 1)
    forward(agp(d_slot, 9))
    agp(flip(d_slot), 0).wait_recv()
    expand((1 - zp) * 2 + 1 - y)
    pass_w(4, "start")
    pass_w(5, "start")

    def shard_of(i):
        zs = jnp.where(zh == 0, i // 2, along_z - 1 - i // 2)
        return zs * 2 + (x if i % 2 == 0 else other)

    def place_of(i, q):
        return (q % 2) * 2 + q // 2 if i % 2 == 0 else q

    def red0(i):
        return remote(part_buf.at[i, 1 - c], r0.at[i], sem_r.at[0, i], rec_r.at[0, i], partner)

    def red1(i):
        far = 1 - y if i % 2 == 0 else 1 - zp
        return remote(
            s1.at[i, pl.ds(2 * far, 2)], r1.at[i], sem_r.at[1, i], rec_r.at[1, i],
            y_peer if i % 2 == 0 else z_peer,
        )

    def red2(i):
        return remote(
            s2.at[i], r2.at[i], sem_r.at[2, i], rec_r.at[2, i], z_peer if i % 2 == 0 else y_peer
        )

    def shrink(i):
        s = shard_of(i)
        if i % 2 == 1:
            for p in range(4, 6):
                arrive_w(p, s // 2)
        for q in range(4):
            value = jnp.dot(hid[q], down_all[s], preferred_element_type=f32).astype(bf16)
            part_buf[i, 0, place_of(i, q)] = value[:own_rows]
            part_buf[i, 1, place_of(i, q)] = value[own_rows:]
        red0(i).start()

    def add0(i):
        red0(i).wait_recv()
        s1[i] = (part_buf[i, c].astype(f32) + r0[i].astype(f32)).astype(bf16)
        red1(i).start()

    def add1(i):
        near, side = (y, zp) if i % 2 == 0 else (zp, y)
        red1(i).wait_recv()
        s2[i] = (s1[i, 2 * near + 1 - side].astype(f32) + r1[i, 1 - side].astype(f32)).astype(bf16)
        red2(i).start()

    def add2(i):
        near, side = (y, zp) if i % 2 == 0 else (zp, y)
        red2(i).wait_recv()
        ffn = s1[i, 2 * near + side].astype(f32) + r1[i, side].astype(f32) + r2[i].astype(f32)
        cols = pl.ds(pl.multiple_of(shard_of(i) * block, block), block)
        result[:, cols] = (mixed[:, cols] + 0.5 * ffn).astype(bf16)

    for i in range(shards + 3):
        if i < shards:
            shrink(i)
        if 0 <= i - 1 < shards:
            add0(i - 1)
        if 0 <= i - 2 < shards:
            add1(i - 2)
        if 0 <= i - 3 < shards:
            add2(i - 3)

    for k in NEAR:
        at_z(k, lambda t: lane_x(t, "wait_send"))
        at_z(k, lambda t: cross_x(t, "wait_send"))
        at_z(k, lambda t: pass_x(t, "wait_send"))
    side_x("wait_send")
    cross_x(z, "wait_send")
    for p in range(pieces):
        send_w(p, "wait_send")
        side_w(p, "wait_send")
        pass_w(p, "wait_send")
    for d in range(1, groups):
        send_out(d, "wait_send")
        send_a(d, "wait_send")
    for d in range(1, shards):
        send_o(lax.rem(me + d, shards)).wait_send()
    for cp in sends:
        cp.wait_send()
    for i in range(shards):
        red0(i).wait_send()
        red1(i).wait_send()
        red2(i).wait_send()


def fast(
    cut, resid, queries, keys, values, cum_gate, out_weight, norm_gain, gate_weight, up_weight, down_weight
):
    rows, width = queries.shape
    heads = cum_gate.shape[1]
    shards = 2 * heads
    two = 2 * HEAD_DIM
    part = rows // 4
    own_rows, model = resid.shape
    groups = rows // own_rows
    depth, hidden = gate_weight.shape
    block = down_weight.shape[1]
    wide = hidden - cut
    g = (cum_gate.T * LOG2E).reshape(heads, rows // 128, 128)
    vmem = pl.BlockSpec(memory_space=pltpu.VMEM)
    hbm = pl.BlockSpec(memory_space=pl.ANY)
    dma = pltpu.SemaphoreType.DMA
    bf16, f32 = jnp.bfloat16, jnp.float32
    return pl.pallas_call(
        functools.partial(layer_kernel, cut),
        in_specs=[vmem] * 6 + [hbm] * 4,
        out_specs=vmem,
        out_shape=jax.ShapeDtypeStruct(resid.shape, bf16),
        scratch_shapes=[
            pltpu.VMEM((heads, rows + 48 + 2 * part, two), bf16),
            pltpu.VMEM((shards, rows + 48 + part, two), bf16),
            pltpu.VMEM((shards, 1, rows), f32),
            pltpu.VMEM((shards, part, two), bf16),
            pltpu.VMEM((shards, part, two), bf16),
            pltpu.VMEM((groups, part, width), bf16),
            pltpu.VMEM((groups, part, width), bf16),
            pltpu.VMEM((groups, width, model), bf16),
            pltpu.VMEM((shards * depth, wide), bf16),
            pltpu.VMEM((shards * depth, wide), bf16),
            pltpu.VMEM((shards, wide, block), bf16),
            pltpu.VMEM((own_rows, model), f32),
            pltpu.VMEM((8, own_rows, model), bf16),
            pltpu.VMEM((4, 2 * own_rows, wide), bf16),
            pltpu.VMEM((shards, 2, 4, own_rows, block), bf16),
            pltpu.VMEM((shards, 4, own_rows, block), bf16),
            pltpu.VMEM((shards, 4, own_rows, block), bf16),
            pltpu.VMEM((shards, 2, own_rows, block), bf16),
            pltpu.VMEM((shards, own_rows, block), bf16),
            pltpu.VMEM((shards, own_rows, block), bf16),
            dma((3, heads)), dma((shards,)), dma((shards,)),
            dma((shards,)), dma((shards,)), dma((groups,)), dma((groups,)),
            dma((groups,)), dma((groups,)),
            dma((6, heads)), dma((6, heads)), dma((6, shards)), dma((6,)),
            dma((10,)), dma((8, 2)), dma((8,)), dma((3, shards)), dma((3, shards)),
        ],
        compiler_params=pltpu.CompilerParams(
            collective_id=0, has_side_effects=True, vmem_limit_bytes=63 * 2**20
        ),
    )(resid, queries, keys, values, g, norm_gain.reshape(1, model), out_weight, gate_weight, up_weight, down_weight)


def rounded(term):
    return term.astype(jnp.bfloat16).astype(jnp.float32)


def flash_kernel(rows, q_block, shard_ref, q_ref, k_ref, v_ref, gate_q_ref, gate_k_ref, out_ref):
    pair = pl.program_id(0)
    block = pl.program_id(1)
    shard = shard_ref[0]
    q = q_ref[...]
    lane = lax.broadcasted_iota(jnp.int32, (q_block, 2 * HEAD_DIM), 1)
    low = lane < HEAD_DIM
    zero = jnp.zeros_like(q)
    q_heads = (jnp.where(low, q, zero), jnp.where(low, zero, q))
    gate_q = gate_q_ref[...]
    gate_lane = lax.broadcasted_iota(jnp.int32, gate_q.shape, 1)
    gates = tuple(
        jnp.sum(jnp.where(gate_lane == 2 * pair + h, gate_q, 0.0), axis=1, keepdims=True) * LOG2E
        for h in range(2)
    )
    scale = HEAD_DIM ** (-0.5) * LOG2E

    def step(j, state, masked):
        best, total, numer = state
        start = pl.multiple_of(j * rows, rows)
        k = k_ref[pl.ds(start, rows), :]
        v = v_ref[pl.ds(start, rows), :]
        new_best, new_total, parts, decay = [], [], [], []
        for h in range(2):
            s = lax.dot_general(
                q_heads[h], k, (((1,), (1,)), ((), ())), preferred_element_type=jnp.float32
            )
            gate_k = gate_k_ref[j, 0, h : h + 1, :] * LOG2E
            s = s * scale + (gates[h] - gate_k)
            if masked:
                row = lax.broadcasted_iota(jnp.int32, s.shape, 0) + block * q_block
                col = lax.broadcasted_iota(jnp.int32, s.shape, 1)
                s = jnp.where(col <= row, s, -1e30)
            top = jnp.maximum(best[h], jnp.max(s, axis=1, keepdims=True))
            keep = jnp.exp2(best[h] - top)
            w = jnp.exp2(s - top)
            new_best.append(top)
            new_total.append(total[h] * keep + jnp.sum(w, axis=1, keepdims=True))
            parts.append(
                lax.dot_general(
                    w.astype(jnp.bfloat16), v, (((1,), (0,)), ((), ())),
                    preferred_element_type=jnp.float32,
                )
            )
            decay.append(keep)
        numer = numer * jnp.where(low, decay[0], decay[1]) + jnp.where(low, parts[0], parts[1])
        return tuple(new_best), tuple(new_total), numer

    column = jnp.zeros((q_block, 1), jnp.float32)
    state = (
        (column - 1e30, column - 1e30),
        (column, column),
        jnp.zeros((q_block, 2 * HEAD_DIM), jnp.float32),
    )
    state = step(shard, state, True)
    state = lax.fori_loop(0, shard, lambda j, s: step(j, s, False), state)
    _, total, numer = state
    out_ref[...] = (numer / jnp.where(low, total[0], total[1])).astype(jnp.bfloat16)


def flash(shard, queries, kv_all, cum_gate, gates_all):
    rows, width = queries.shape
    pairs = width // (2 * HEAD_DIM)
    count = kv_all.shape[0]
    shards = count // rows
    heads = cum_gate.shape[1]
    q_block = 256 if rows % 256 == 0 else rows
    two = 2 * HEAD_DIM
    gates_all = gates_all.reshape(shards, pairs, 2, rows)
    return pl.pallas_call(
        functools.partial(flash_kernel, rows, q_block),
        grid=(pairs, rows // q_block),
        in_specs=[
            pl.BlockSpec(memory_space=pltpu.SMEM),
            pl.BlockSpec((q_block, two), lambda p, i: (i, p)),
            pl.BlockSpec((count, two), lambda p, i: (0, p)),
            pl.BlockSpec((count, two), lambda p, i: (0, pairs + p)),
            pl.BlockSpec((q_block, heads), lambda p, i: (i, 0)),
            pl.BlockSpec((shards, 1, 2, rows), lambda p, i: (0, p, 0, 0)),
        ],
        out_specs=pl.BlockSpec((q_block, two), lambda p, i: (i, p)),
        out_shape=jax.ShapeDtypeStruct((rows, width), jnp.bfloat16),
        compiler_params=pltpu.CompilerParams(vmem_limit_bytes=40 * 2**20),
        cost_estimate=pl.CostEstimate(
            flops=8 * rows * count * width,
            bytes_accessed=4 * count * width,
            transcendentals=rows * count * width // HEAD_DIM,
        ),
    )(shard.reshape(1), queries, kv_all, kv_all, cum_gate, gates_all)


def shift(value, axis, size, step):
    return lax.ppermute(value, axis, [(i, (i + step) % size) for i in range(size)])


def exchange(weight, split, joined, size):
    here = lax.axis_index("x")
    width = weight.shape[split] // size
    pieces = []
    for step in range(size):
        target = lax.rem(here + step, size)
        piece = lax.dynamic_slice_in_dim(weight, target * width, width, split)
        pieces.append(piece if step == 0 else shift(piece, "x", size, step))
    if size == 1:
        return pieces[0]
    if size == 2:
        first = here == 0
        return jnp.concatenate(
            [jnp.where(first, pieces[0], pieces[1]), jnp.where(first, pieces[1], pieces[0])], joined
        )
    length = weight.shape[joined]
    shape = list(pieces[0].shape)
    shape[joined] = length * size
    whole = jnp.zeros(shape, weight.dtype)
    for step in range(size):
        source = lax.rem(here - step + size, size)
        whole = lax.dynamic_update_slice_in_dim(whole, pieces[step], source * length, joined)
    return whole


def local(
    resid,
    queries,
    keys,
    values,
    cum_gate,
    out_weight,
    norm_gain,
    gate_weight,
    up_weight,
    down_weight,
):
    along_x = lax.axis_size("x")
    groups = lax.axis_size("tp")
    shard = lax.axis_index("z") * along_x + lax.axis_index("x")
    gates_all = lax.all_gather(cum_gate.T, ("z", "x"), axis=0)
    kv_all = lax.all_gather(jnp.concatenate([keys, values], axis=1), ("z", "x"), axis=0, tiled=True)
    proj_weights = [out_weight] + [shift(out_weight, "tp", groups, d) for d in range(1, groups)]
    gate_cols = exchange(gate_weight, 1, 0, along_x)
    up_cols = exchange(up_weight, 1, 0, along_x)
    down_rows = exchange(down_weight, 0, 1, along_x)
    along_z = lax.axis_size("z")
    gate_full = lax.all_gather(gate_cols, "z", axis=0, tiled=True)
    up_full = lax.all_gather(up_cols, "z", axis=0, tiled=True)
    down_parts = [down_rows] + [shift(down_rows, "z", along_z, d) for d in range(1, along_z)]

    queries, gate_cols, up_cols, down_rows = lax.optimization_barrier(
        (queries, gate_cols, up_cols, down_rows)
    )
    attn = flash(shard.astype(jnp.int32), queries, kv_all, cum_gate, gates_all)

    own_rows = lax.all_to_all(attn, "tp", split_axis=0, concat_axis=1, tiled=True)
    width = attn.shape[1]
    here = lax.axis_index("tp")
    mixed = resid.astype(jnp.float32)
    for d in range(groups):
        group = lax.rem(here - d + groups, groups)
        part = lax.dynamic_slice_in_dim(own_rows, group * width, width, 1)
        mixed = mixed + rounded(
            jnp.dot(part, proj_weights[d], preferred_element_type=jnp.float32)
        )
    normed, up_full = lax.optimization_barrier((rms_norm(mixed, norm_gain), up_full))
    normed_all = lax.all_gather(normed, ("x", "tp"), axis=0, tiled=True)
    gate_sum = jnp.dot(normed_all, gate_full, preferred_element_type=jnp.float32)
    up_sum = jnp.dot(normed_all, up_full, preferred_element_type=jnp.float32)
    hidden = (jax.nn.silu(gate_sum) * up_sum).astype(jnp.bfloat16)
    ffn_part = jnp.concatenate(
        [
            jnp.dot(hidden, part, preferred_element_type=jnp.float32).astype(jnp.bfloat16)
            for part in down_parts
        ],
        axis=1,
    )
    turned = lax.psum_scatter(ffn_part, ("x", "tp"), scatter_dimension=0, tiled=True)
    block = down_parts[0].shape[1]
    ffn = jnp.concatenate(
        [
            lax.dynamic_slice_in_dim(
                turned, lax.rem(lax.axis_index("z") - c + along_z, along_z) * block, block, 1
            )
            for c in range(along_z)
        ],
        axis=1,
    ).astype(jnp.float32)
    return (mixed + 0.5 * ffn).astype(jnp.bfloat16)


def general(mesh):
    along_sp = mesh.shape["sp"]
    along_x = 2 if along_sp % 2 == 0 else 1
    grid = Mesh(
        mesh.devices.reshape(along_sp // along_x, along_x, mesh.shape["tp"]), ("z", "x", "tp")
    )
    sp = ("z", "x")
    in_specs = (
        P(("z", "x", "tp"), None),
        P(sp, "tp"),
        P(sp, "tp"),
        P(sp, "tp"),
        P(sp, "tp"),
        P("tp", None),
        P(),
        P(sp, "tp"),
        P(sp, "tp"),
        P("tp", sp),
    )
    out_specs = P(("z", "x", "tp"), None)

    return jax.shard_map(local, mesh=grid, in_specs=in_specs, out_specs=out_specs, check_vma=False)


def solution(mesh):
    along_sp, along_tp = mesh.shape["sp"], mesh.shape["tp"]
    slow = general(mesh)

    def run(*args):
        heads = args[4].shape[1] // along_tp
        rows = args[1].shape[0] // along_sp
        hidden = args[7].shape[1] // along_tp
        cut = hidden // 2 // 128 * 128
        if along_sp != 2 * heads or heads != 4 or along_tp != 4 or rows % 256 or rows > 2048 or cut == 0:
            return slow(*args)
        grid = Mesh(mesh.devices.reshape(heads // 2, 2, 2, along_tp // 2, 2), AXES)
        sp, tp = ("zh", "zp", "x"), ("y", "c")
        in_specs = (
            P(sp + tp, None),
            P(sp, tp), P(sp, tp), P(sp, tp), P(sp, tp),
            P(tp, None),
            P(),
            P(sp, tp), P(sp, tp), P(tp, sp),
        )
        step = jax.shard_map(
            functools.partial(fast, cut), mesh=grid, in_specs=in_specs,
            out_specs=P(sp + tp, None), check_vma=False,
        )
        return step(*args)

    return run
```
